32 devices in a mesh: sp: 4 (over y, x), tp: 8 (over z, core).
Axes of the slice: x: 2, y: 2, z: 4, core: 2. Of those that a mesh axis runs over, the one named last changes fastest.
Arguments:
- conv_outer: bfloat16 [2048, 1024], P('tp', 'sp'), may hold values from -6 to 6
- conv_inner: bfloat16 [2048, 1024], P('tp', 'sp'), may hold values from -6 to 6
- conv_input: bfloat16 [2048, 1024], P('tp', 'sp'), may hold values from -6 to 6
- conv_taps: float32 [3, 2048], P(None, 'tp'), may hold values from -3 to 3
- out_proj: bfloat16 [2048, 4096], P('tp'), may hold values from -0.125 to 0.125
- mixed_state: bfloat16 [1024, 4096], P('sp', 'tp'), may hold values from -6 to 6
- route_ids: int32 [1024, 2], P('sp'), may hold values from 0 to 3, all different within a row; in each aligned block of 256 rows (0 to 255, 256 to 511, ...) at most 256 rows name the same one
- route_weights: float32 [1024, 2], P('sp'), may hold values from 0.1 to 1
- w_gate: bfloat16 [4, 2048, 4096], P('sp', 'tp'), may hold values from -0.09375 to 0.09375
- w_up: bfloat16 [4, 2048, 4096], P('sp', 'tp'), may hold values from -0.09375 to 0.09375
- w_down: bfloat16 [4, 2048, 4096], P('sp', 'tp'), may hold values from -0.125 to 0.125
- cotangent: bfloat16 [1024, 4096], P('sp', 'tp'), may hold values from -8 to 8
Outputs:
- grad_gate: float32 [4, 2048, 4096], P('sp', 'tp')
- grad_up: float32 [4, 2048, 4096], P('sp', 'tp')
- grad_down: float32 [4, 2048, 4096], P('sp', 'tp')
- grad_mixed: bfloat16 [1024, 4096], P('sp', 'tp')
- grad_proj: float32 [2048, 4096], P('tp', 'sp')
- grad_outer: bfloat16 [2048, 1024], P('tp', 'sp')
- grad_inner: bfloat16 [2048, 1024], P('tp', 'sp')
- grad_input: bfloat16 [2048, 1024], P('tp', 'sp')
The draws below stay inside these ranges and needn't reach their ends.
Inputs may be any that keep to these rules, and one draw needn't show every extreme that they name: `route_ids`: each row names 2 different experts; among the tokens of one index of sp no expert is named more than 256 times, a bound that some block reaches.
All inputs are finite; a program needn't handle non-finite values.
Results may differ from the reference program's by a relative error of at most 0.022.
Values may be sent and summed in bfloat16 or wider, within the bound.
A program may use at most 128 MiB of HBM per device.

```python
import math
import jax
import jax.numpy as jnp
import numpy as np
from jax import lax

D = 4096
FF = 2048
CH = 2048
TAPS = 3
TOP = 2
TOK_DEV = 256
EXPERTS = 4
CAP = 256
TOKENS = 1024
N_SP = 4
N_TP = 8


def with_spikes(result, rng, source, target, blocks, factor):
    def block_of(dim):
        return (jnp.arange(result.shape[dim]) // (result.shape[dim] // blocks)).reshape((-1,) + (1,) * (result.ndim - 1 - dim))

    near = jax.random.permutation(rng, blocks)[block_of(target)]
    other_side = (block_of(target) + blocks // 2) % blocks
    return jnp.where((block_of(source) == near) | (block_of(source) == other_side), factor * result, result)


def level_of(stream_key, dims, cuts, least, top_value):
    def one(axis_at, shards_of):
        heights = jax.random.uniform(jax.random.fold_in(jax.random.fold_in(stream_key, 6), axis_at), (shards_of,), jnp.float32, least / len(cuts), top_value / len(cuts))
        return jnp.repeat(jnp.exp(heights), dims[axis_at] // shards_of).reshape((-1,) + (1,) * (len(dims) - axis_at - 1))

    factor_of = one(*cuts[0])
    for cut in cuts[1:]:
        factor_of = factor_of * one(*cut)
    return factor_of


def shared_out(stream_key, own, number, rows, amount, top, most, lean):
    ranking = jax.random.permutation(stream_key, amount)
    packed, ordinary = load_shares(amount, rows * top, most, lean, True), load_shares(amount, rows * top, most, lean, False)
    places = jnp.arange(amount)

    def named(lengths, rotation):
        used = int((lengths > 0).sum())
        fixed = max(1, used // 4)
        shifted = fixed + (places - fixed + rotation * (used - fixed)) % max(1, amount - fixed)
        return jnp.zeros((amount,), jnp.int32).at[ranking[jnp.where(places < fixed, places, shifted)]].set(jnp.asarray(lengths, jnp.int32))

    lengths = jnp.where(number % 4 == 0, named(packed, number // 4), named(ordinary, number - number // 4 - 1))
    mixed = jax.random.permutation(jax.random.fold_in(own, 3), amount)
    giver, taker = mixed[0:amount // 2 * 2:2], mixed[1:amount // 2 * 2:2]
    margin = jnp.minimum(lengths[giver] - 1, most - lengths[taker]) // 2
    margin = jnp.where((giver == ranking[0]) | (taker == ranking[0]) | (lengths[taker] == 0), 0, jnp.maximum(margin, 0))
    shifted = jax.random.randint(jax.random.fold_in(own, 4), (amount // 2,), 0, 1 << 20) % (margin + 1)
    lengths = lengths.at[giver].add(-shifted).at[taker].add(shifted)
    items = jnp.searchsorted(jnp.cumsum(lengths), jnp.arange(rows * top), side="right").astype(jnp.int32)
    grid = items.reshape(top, rows).T
    grid = grid[jax.random.permutation(jax.random.fold_in(own, 1), rows)]
    rotation = jax.random.randint(jax.random.fold_in(own, 2), (rows, 1), 0, top)
    return jnp.take_along_axis(grid, (jnp.arange(top)[None, :] + rotation) % top, axis=1)


def load_shares(number_of, total, most, slope, full):
    loads = [(1 << 20) // math.isqrt(standing ** slope) + 1 for standing in range(1, number_of + 1)]
    largest = most if full else min(most, max(-(-total // number_of), total * loads[0] // sum(loads)))
    least = 1 if total - largest >= number_of - 1 else 0
    holding, surplus = [largest] + [least] * (number_of - 1), total - largest - least * (number_of - 1)
    while surplus > 0:
        free = [i for i in range(1, number_of) if holding[i] < largest] or [i for i in range(1, number_of) if holding[i] < most]
        pool, left = sum([loads[i] for i in free]), surplus
        for i in free:
            extra = min(most - holding[i], max(1, left * loads[i] // pool), surplus)
            holding[i] = holding[i] + extra
            surplus = surplus - extra
    return np.array(holding)


def centred(key, extent, scale, limit, split=(), kind=jnp.bfloat16):
    values = jax.random.normal(key, extent, jnp.float32) * scale
    if len(split) > 0:
        values = level_of(key, extent, split, -0.22, 0.18) * values
    return jnp.clip(values, min=-limit, max=limit).astype(kind)


def noise_with(key, shape, spread, most, split, heavy, held_as=jnp.bfloat16):
    drawn = spread * jax.random.normal(key, shape, jnp.float32)
    if split:
        drawn = drawn * level_of(key, shape, split, -0.22, 0.18)
    return jnp.clip(with_spikes(drawn, jax.random.fold_in(key, 3), *heavy), -most, most).astype(held_as)


def setup_inputs(seed: int = 0) -> dict:
    arg_keys = jax.random.split(jax.random.key(seed), 13)
    conv_outer = centred(arg_keys[0], (CH, TOKENS), 1.0, 6.0, ((0, 8), (1, 4)))
    conv_inner = centred(arg_keys[1], (CH, TOKENS), 1.0, 6.0, ((0, 8), (1, 4)))
    conv_input = centred(arg_keys[2], (CH, TOKENS), 1.0, 6.0, ((0, 8), (1, 4)))
    conv_taps = centred(arg_keys[3], (TAPS, CH), 0.6, 3.0, ((1, 8),), jnp.float32)
    out_proj = centred(arg_keys[4], (CH, D), CH ** -0.5, 0.125, ((0, 8),))
    mixed_state = centred(arg_keys[5], (TOKENS, D), 1.0, 6.0, ((0, 4), (1, 8)))
    route_ids_keys = jax.random.split(jax.random.fold_in(arg_keys[6], 1), TOKENS // TOK_DEV)
    route_ids_turns = jax.random.permutation(jax.random.fold_in(arg_keys[6], 3), TOKENS // TOK_DEV)
    route_ids = jax.vmap(lambda own, number: shared_out(jax.random.fold_in(arg_keys[6], 2), own, number, TOK_DEV, EXPERTS, TOP, CAP, 2))(route_ids_keys, route_ids_turns).reshape((TOKENS, TOP))
    route_weights = jnp.clip(0.1 + 0.9 * jax.random.uniform(arg_keys[7], (TOKENS, TOP), jnp.float32) ** level_of(arg_keys[7], (TOKENS, TOP), ((0, 4),), -0.2, 0.2), 0.1, 1.0)
    w_gate = centred(arg_keys[8], (EXPERTS, FF, D), D ** -0.5, 0.09375, ((0, 4), (1, 8)))
    w_up = centred(arg_keys[9], (EXPERTS, FF, D), D ** -0.5, 0.09375, ((0, 4), (1, 8)))
    w_down = centred(arg_keys[10], (EXPERTS, FF, D), FF ** -0.5, 0.125, ((0, 4), (1, 8)))
    cotangent = noise_with(arg_keys[11], (TOKENS, D), 1.0, 8.0, ((0, 4), (1, 8)), (0, 1, 8, 2.0))
    return {"conv_outer": conv_outer, "conv_inner": conv_inner, "conv_input": conv_input, "conv_taps": conv_taps, "out_proj": out_proj, "mixed_state": mixed_state, "route_ids": route_ids, "route_weights": route_weights, "w_gate": w_gate, "w_up": w_up, "w_down": w_down, "cotangent": cotangent}


def expert_core(rows_in, rows_grad, gate_w, up_w, down_w):
    gate_pre = jnp.dot(rows_in, gate_w.T, preferred_element_type=jnp.float32)
    up_pre = jnp.dot(rows_in, up_w.T, preferred_element_type=jnp.float32)
    sig_gate = jax.nn.sigmoid(gate_pre)
    silu_gate = gate_pre * sig_gate
    hidden = (silu_gate * up_pre).astype(jnp.bfloat16)
    back_hidden = jnp.dot(rows_grad, down_w.T, preferred_element_type=jnp.float32)
    back_gate = (back_hidden * up_pre * sig_gate * (1.0 + gate_pre * (1.0 - sig_gate))).astype(jnp.bfloat16)
    back_up = (back_hidden * silu_gate).astype(jnp.bfloat16)
    grad_down_e = jnp.dot(hidden.T, rows_grad, preferred_element_type=jnp.float32)
    grad_gate_e = jnp.dot(back_gate.T, rows_in, preferred_element_type=jnp.float32)
    grad_up_e = jnp.dot(back_up.T, rows_in, preferred_element_type=jnp.float32)
    return back_gate, back_up, grad_gate_e, grad_up_e, grad_down_e


def reference(conv_outer, conv_inner, conv_input, conv_taps, out_proj, mixed_state, route_ids, route_weights, w_gate, w_up, w_down, cotangent):
    block_ids = route_ids.reshape(N_SP, TOP * TOK_DEV)
    onehot = (block_ids[:, :, None] == jnp.arange(EXPERTS, dtype=jnp.int32)[None, None, :]).astype(jnp.int32)
    position = jnp.sum(jnp.cumsum(onehot, axis=1) * onehot, axis=2) - 1
    device_ids = jnp.broadcast_to(jnp.arange(N_SP, dtype=jnp.int32)[:, None], block_ids.shape)
    assign = jnp.arange(N_SP * TOP * TOK_DEV, dtype=jnp.int32).reshape(N_SP, TOP * TOK_DEV)
    table = jnp.full((EXPERTS, N_SP, CAP), -1, jnp.int32).at[block_ids, device_ids, position].set(assign)
    table = table.reshape(EXPERTS, N_SP * CAP)
    weight_flat = route_weights.reshape(-1)

    def expert_pass(operands):
        table_row, gate_w, up_w, down_w = operands
        valid = table_row >= 0
        safe_idx = jnp.where(valid, table_row, 0)
        token_idx = safe_idx // TOP
        rows_in = jnp.where(valid[:, None], mixed_state[token_idx], jnp.zeros((), jnp.bfloat16))
        scale = jnp.where(valid, weight_flat[safe_idx], jnp.zeros((), jnp.float32))
        rows_grad = (cotangent[token_idx].astype(jnp.float32) * scale[:, None]).astype(jnp.bfloat16)
        back_gate, back_up, grad_gate_e, grad_up_e, grad_down_e = expert_core(rows_in, rows_grad, gate_w, up_w, down_w)
        row_count = rows_in.shape[0]
        gate_blocks = back_gate.astype(jnp.float32).reshape(row_count, N_TP, FF // N_TP)
        up_blocks = back_up.astype(jnp.float32).reshape(row_count, N_TP, FF // N_TP)
        gate_wblk = gate_w.astype(jnp.float32).reshape(N_TP, FF // N_TP, D)
        up_wblk = up_w.astype(jnp.float32).reshape(N_TP, FF // N_TP, D)
        partial_value = jnp.einsum("rbf,bfd->brd", gate_blocks, gate_wblk) + jnp.einsum("rbf,bfd->brd", up_blocks, up_wblk)
        rounded = lax.optimization_barrier(partial_value.astype(jnp.bfloat16))
        row_back = jnp.sum(rounded.astype(jnp.float32), axis=0).astype(jnp.bfloat16)
        return row_back, grad_gate_e, grad_up_e, grad_down_e

    row_back, grad_gate, grad_up, grad_down = lax.map(expert_pass, (table, w_gate, w_up, w_down))
    flat_table = table.reshape(-1)
    valid_all = flat_table >= 0
    token_all = jnp.where(valid_all, flat_table, 0) // TOP
    back_vals = jnp.where(valid_all[:, None], row_back.reshape(-1, D).astype(jnp.float32), jnp.zeros((), jnp.float32))
    moe_grad = jnp.zeros((TOKENS, D), jnp.float32).at[token_all].add(back_vals)
    grad_mixed = (cotangent.astype(jnp.float32) + moe_grad).astype(jnp.bfloat16)

    inner_prod = conv_inner.astype(jnp.float32) * conv_input.astype(jnp.float32)
    padded = jnp.pad(inner_prod, ((0, 0), (TAPS - 1, 0)))
    conv_out = jnp.zeros_like(inner_prod)
    for offset in range(TAPS):
        conv_out = conv_out + conv_taps[offset][:, None] * padded[:, offset:offset + TOKENS]
    mixer_act = (conv_outer.astype(jnp.float32) * conv_out).astype(jnp.bfloat16)
    back_mixer = jnp.dot(out_proj, grad_mixed.T, preferred_element_type=jnp.float32)
    grad_proj = jnp.dot(mixer_act, grad_mixed, preferred_element_type=jnp.float32)
    grad_outer = (back_mixer * conv_out).astype(jnp.bfloat16)
    back_conv = back_mixer * conv_outer.astype(jnp.float32)
    padded_back = jnp.pad(back_conv, ((0, 0), (0, TAPS - 1)))
    back_prod = jnp.zeros_like(back_conv)
    for offset in range(TAPS):
        shift_by = TAPS - 1 - offset
        back_prod = back_prod + conv_taps[offset][:, None] * padded_back[:, shift_by:shift_by + TOKENS]
    grad_inner = (back_prod * conv_input.astype(jnp.float32)).astype(jnp.bfloat16)
    grad_input = (back_prod * conv_inner.astype(jnp.float32)).astype(jnp.bfloat16)
    return grad_gate, grad_up, grad_down, grad_mixed, grad_proj, grad_outer, grad_inner, grad_input
```

```python
import functools

import jax
import jax.numpy as jnp
from jax import lax
from jax.experimental import pallas as pl
from jax.experimental.pallas import tpu as pltpu
from jax.sharding import PartitionSpec as P


def from_behind(value, axis, steps):
    count = lax.axis_size(axis)
    first, last = (max(0, -steps), min(count, count - steps))
    return lax.ppermute(value, axis, [(source, source + steps) for source in range(first, last)])


def row_back_kernel(gate_ref, up_ref, gate_w_ref, up_w_ref, out_ref):
    total = jnp.dot(gate_ref[...], gate_w_ref[...], preferred_element_type=jnp.float32)
    total += jnp.dot(up_ref[...], up_w_ref[...], preferred_element_type=jnp.float32)
    out_ref[...] = total.astype(out_ref.dtype)


def row_back(back_gate, back_up, gate_w, up_w):
    rows, hidden = back_gate.shape
    width = gate_w.shape[1]
    tile = min(512, width)
    left = pl.BlockSpec((rows, hidden), lambda i: (0, 0))
    right = pl.BlockSpec((hidden, tile), lambda i: (0, i))
    return pl.pallas_call(
        row_back_kernel,
        grid=(width // tile,),
        out_shape=jax.ShapeDtypeStruct((rows, width), jnp.bfloat16),
        in_specs=[left, left, right, right],
        out_specs=pl.BlockSpec((rows, tile), lambda i: (0, i)),
        cost_estimate=pl.CostEstimate(
            flops=4 * rows * hidden * width,
            bytes_accessed=2 * (2 * rows * hidden + 2 * hidden * width + rows * width),
            transcendentals=0,
        ),
        name="row_back",
    )(back_gate, back_up, gate_w, up_w)


def expert_step(rows_in, rows_grad, gate_w, up_w, down_w):
    gate_pre = jnp.einsum("rd,fd->rf", rows_in, gate_w, preferred_element_type=jnp.float32)
    up_pre = jnp.einsum("rd,fd->rf", rows_in, up_w, preferred_element_type=jnp.float32)
    sig_gate = jax.nn.sigmoid(gate_pre)
    silu_gate = gate_pre * sig_gate
    hidden = (silu_gate * up_pre).astype(jnp.bfloat16)
    back_hidden = jnp.einsum("rd,fd->rf", rows_grad, down_w, preferred_element_type=jnp.float32)
    back_gate = (back_hidden * up_pre * sig_gate * (1.0 + gate_pre * (1.0 - sig_gate))).astype(
        jnp.bfloat16
    )
    back_up = (back_hidden * silu_gate).astype(jnp.bfloat16)
    grad_down_e = jnp.einsum("rf,rd->fd", hidden, rows_grad, preferred_element_type=jnp.float32)
    grad_gate_e = jnp.einsum("rf,rd->fd", back_gate, rows_in, preferred_element_type=jnp.float32)
    grad_up_e = jnp.einsum("rf,rd->fd", back_up, rows_in, preferred_element_type=jnp.float32)
    partial_value = row_back(back_gate, back_up, gate_w, up_w)
    return (partial_value, grad_gate_e, grad_up_e, grad_down_e)


Z_UP, Z_DOWN, BY_X, BY_Y, HALF_X, HALF_Y, PEER = range(7)
KINDS = PEER + 4


def gather_kernel(levels, cot_in, state_in, cot_out, state_out, own_sem, send_sem, recv_sem):
    sp, tp = lax.axis_index("sp"), lax.axis_index("tp")
    level, core = tp // 2, tp % 2
    beside_x = sp + 1 - 2 * (sp % 2)
    beside_y = (sp + 2) % 4
    across = 3 - sp
    peer = tp + 1 - 2 * core
    rows, cols = cot_in.shape
    half = rows // 2
    ins, outs = (cot_in, state_in), (cot_out, state_out)

    barrier = pltpu.get_barrier_semaphore()

    def greet(to_sp, to_tp):
        pl.semaphore_signal(
            barrier,
            inc=1,
            device_id=(to_sp, to_tp),
            device_id_type=pl.DeviceIdType.MESH,
        )

    greet(beside_x, tp)
    greet(beside_y, tp)
    greet(sp, peer)
    pl.when(level > 0)(lambda: greet(sp, tp - 2))
    pl.when(level < levels - 1)(lambda: greet(sp, tp + 2))
    one = jnp.int32(1)
    none = jnp.int32(0)
    pl.semaphore_wait(
        barrier,
        3 + jnp.where(level > 0, one, none) + jnp.where(level < levels - 1, one, none),
    )

    def block(array, of_sp, of_level, of_core, start=0, size=rows):
        return outs[array].at[
            pl.ds(pl.multiple_of(of_sp * rows + start, 16), size),
            pl.ds(pl.multiple_of((of_level * 2 + of_core) * cols, 128), cols),
        ]

    def remote(array, kind, of_level, source, target, to_sp, to_tp):
        return pltpu.make_async_remote_copy(
            src_ref=source,
            dst_ref=target,
            send_sem=send_sem.at[array, kind, of_level],
            recv_sem=recv_sem.at[array, kind, of_level],
            device_id=(to_sp, to_tp),
            device_id_type=pl.DeviceIdType.MESH,
        )

    def spread(array, of_level, source, kind, to_sp, to_tp):
        remote(
            array, kind, of_level, source, block(array, sp, of_level, core), to_sp, to_tp
        ).start()

    def pieces(array, of_level):
        return {
            Z_UP: block(array, sp, of_level, core),
            Z_DOWN: block(array, sp, of_level, core),
            BY_X: block(array, beside_x, of_level, core),
            BY_Y: block(array, beside_y, of_level, core),
            HALF_Y: block(array, across, of_level, core, 0, half),
            HALF_X: block(array, across, of_level, core, half, half),
            PEER: block(array, sp, of_level, 1 - core),
            PEER + 1: block(array, beside_x, of_level, 1 - core),
            PEER + 2: block(array, beside_y, of_level, 1 - core),
            PEER + 3: block(array, across, of_level, 1 - core),
        }

    def arrive(array, kind, of_level):
        piece = pieces(array, of_level)[kind]
        remote(array, kind, of_level, piece, piece, sp, peer).wait_recv()

    def left(array, kind, of_level):
        piece = pieces(array, of_level)[kind]
        remote(array, kind, of_level, piece, piece, sp, peer).wait_send()

    def hand_on(array, of_level, kind, of_sp, to_sp, to_tp, start=0, size=rows):
        piece = block(array, of_sp, of_level, core, start, size)
        remote(array, kind, of_level, piece, piece, to_sp, to_tp).start()

    def column(array, step, up):
        of_level = level if step == 0 else (level - step if up else level + step)
        if step == 0:
            source = ins[array]
            pltpu.make_async_copy(
                source, block(array, sp, level, core), own_sem.at[array]
            ).start()
        else:
            arrive(array, Z_UP if up else Z_DOWN, of_level)
            source = block(array, sp, of_level, core)
        if step == 0 or up:
            pl.when(level < levels - 1)(
                lambda: spread(array, of_level, source, Z_UP, sp, tp + 2)
            )
        if step == 0 or not up:
            pl.when(level > 0)(lambda: spread(array, of_level, source, Z_DOWN, sp, tp - 2))
        spread(array, of_level, source, BY_X, beside_x, tp)
        spread(array, of_level, source, BY_Y, beside_y, tp)
        spread(array, of_level, source, PEER, sp, peer)

    def plane(array, step, up):
        of_level = level - step if up else level + step
        arrive(array, BY_X, of_level)
        hand_on(array, of_level, HALF_Y, beside_x, beside_y, tp, 0, half)
        hand_on(array, of_level, PEER + 1, beside_x, sp, peer)
        arrive(array, BY_Y, of_level)
        hand_on(array, of_level, HALF_X, beside_y, beside_x, tp, half, half)
        hand_on(array, of_level, PEER + 2, beside_y, sp, peer)

    def corner(array, step, up):
        of_level = level - step if up else level + step
        arrive(array, HALF_X, of_level)
        arrive(array, HALF_Y, of_level)
        hand_on(array, of_level, PEER + 3, across, sp, peer)

    def each(action, step):
        if not 0 <= step < levels:
            return
        if step == 0:
            for array in range(2):
                action(array, 0, True)
            return

        @pl.when(level >= step)
        def _():
            for array in range(2):
                action(array, step, True)

        @pl.when(level < levels - step)
        def _():
            for array in range(2):
                action(array, step, False)

    for step in range(levels + 2):
        each(column, step)
        each(plane, step - 1)
        each(corner, step - 2)

    for array in range(2):
        pltpu.make_async_copy(
            ins[array], block(array, sp, level, core), own_sem.at[array]
        ).wait()
        for of_level in range(levels):
            for kind in (PEER, PEER + 1, PEER + 2, PEER + 3):
                arrive(array, kind, of_level)
                left(array, kind, of_level)
            for kind in (BY_X, BY_Y, HALF_X, HALF_Y):
                left(array, kind, of_level)
            pl.when((level < levels - 1) & (level >= of_level))(
                lambda: left(array, Z_UP, of_level)
            )
            pl.when((level > 0) & (level <= of_level))(lambda: left(array, Z_DOWN, of_level))


def gather_all(cotangent, mixed_state):
    rows, cols = cotangent.shape
    levels = lax.axis_size("tp") // 2
    whole = jax.ShapeDtypeStruct((4 * rows, 2 * levels * cols), cotangent.dtype)
    return pl.pallas_call(
        functools.partial(gather_kernel, levels),
        out_shape=(whole, whole),
        in_specs=[pl.BlockSpec(memory_space=pltpu.VMEM)] * 2,
        out_specs=[pl.BlockSpec(memory_space=pl.ANY)] * 2,
        scratch_shapes=[
            pltpu.SemaphoreType.DMA((2,)),
            pltpu.SemaphoreType.DMA((2, KINDS, levels)),
            pltpu.SemaphoreType.DMA((2, KINDS, levels)),
        ],
        compiler_params=pltpu.CompilerParams(collective_id=0, has_side_effects=True),
        name="gather_all",
    )(cotangent, mixed_state)


def sum_blocks(tall, sp_size, rows, cols):
    parts = lax.all_to_all(
        tall.reshape(sp_size, 1, rows, cols), "sp", split_axis=0, concat_axis=0, tiled=True
    )
    return jnp.sum(parts.reshape(sp_size, rows, cols).astype(jnp.float32), axis=0)


def shards(
    conv_outer,
    conv_inner,
    conv_input,
    conv_taps,
    out_proj,
    mixed_state,
    route_ids,
    route_weights,
    w_gate,
    w_up,
    w_down,
    cotangent,
):
    tok_count = mixed_state.shape[0]
    col_count = mixed_state.shape[1]
    top_count = route_ids.shape[1]
    sp_size = lax.axis_size("sp")
    local_experts = w_gate.shape[0]
    experts = local_experts * sp_size
    capacity = 4 * tok_count // experts
    if capacity == tok_count and sp_size == 4 and lax.axis_size("tp") % 2 == 0:
        choice = route_ids[:, :, None] == jnp.arange(experts, dtype=jnp.int32)[None, None, :]
        scale_of = jnp.sum(jnp.where(choice, route_weights[:, :, None], 0.0), axis=1).T
        scales = lax.all_to_all(
            scale_of[:, None], "sp", split_axis=0, concat_axis=1, tiled=True
        ).reshape(-1, 1)
        cot_all, rows_in = gather_all(cotangent, mixed_state)
        rows_grad = (cot_all.astype(jnp.float32) * scales).astype(jnp.bfloat16)
        partial_value, grad_gate_e, grad_up_e, grad_down_e = expert_step(
            rows_in, rows_grad, w_gate[0], w_up[0], w_down[0]
        )
        tall = lax.psum_scatter(
            partial_value, "tp", scatter_dimension=1, tiled=True
        )
        tall, grad_gate_e, grad_up_e, grad_down_e = lax.optimization_barrier(
            (tall, grad_gate_e, grad_up_e, grad_down_e)
        )
        summed = sum_blocks(tall, sp_size, tok_count, col_count)
        grad_mixed = (cotangent.astype(jnp.float32) + summed).astype(jnp.bfloat16)
    else:
        flat_ids = route_ids.reshape(-1)
        onehot = (flat_ids[:, None] == jnp.arange(experts, dtype=jnp.int32)[None, :]).astype(jnp.int32)
        slot_pos = jnp.sum(jnp.cumsum(onehot, axis=0) * onehot, axis=1) - 1
        slot_dest = flat_ids * capacity + slot_pos
        token_of = jnp.arange(flat_ids.shape[0], dtype=jnp.int32) // top_count
        scale_flat = route_weights.reshape(-1)[:, None]

        def pack_rows(rows):
            buffer = jnp.zeros((experts * capacity, rows.shape[1]), rows.dtype).at[slot_dest].set(rows)
            return buffer.reshape(sp_size, local_experts, capacity, rows.shape[1])

        sent_state = pack_rows(mixed_state[token_of])
        sent_grad = pack_rows(
            (cotangent[token_of].astype(jnp.float32) * scale_flat).astype(jnp.bfloat16)
        )
        recv_state, recv_grad = (
            lax.all_to_all(sent_state, "sp", split_axis=0, concat_axis=0, tiled=True),
            lax.all_to_all(sent_grad, "sp", split_axis=0, concat_axis=0, tiled=True),
        )
        state_rows, grad_rows = (
            lax.all_gather(recv_state[:, 0], "tp", axis=2, tiled=True),
            lax.all_gather(recv_grad[:, 0], "tp", axis=2, tiled=True),
        )
        width = state_rows.shape[2]
        rows_in = state_rows.reshape(-1, width)
        rows_grad = grad_rows.reshape(-1, width)
        partial_value, grad_gate_e, grad_up_e, grad_down_e = expert_step(
            rows_in, rows_grad, w_gate[0], w_up[0], w_down[0]
        )
        summed = lax.psum_scatter(
            partial_value, "tp", scatter_dimension=1, tiled=True
        )
        back_rows = summed.reshape(sp_size, capacity, col_count)
        arrived = lax.all_to_all(
            back_rows[:, None], "sp", split_axis=0, concat_axis=0, tiled=True
        ).reshape(experts * capacity, col_count)
        picked = arrived[slot_dest].astype(jnp.float32).reshape(tok_count, top_count, col_count)
        grad_mixed = (cotangent.astype(jnp.float32) + jnp.sum(picked, axis=1)).astype(jnp.bfloat16)
    taps_count = conv_taps.shape[0]
    rim_width = taps_count - 1
    head_block = from_behind(
        jnp.stack([conv_inner[:, tok_count - rim_width :], conv_input[:, tok_count - rim_width :]]),
        "sp",
        1,
    )
    inner_ext = jnp.concatenate([head_block[0], conv_inner], axis=1).astype(jnp.float32)
    input_ext = jnp.concatenate([head_block[1], conv_input], axis=1).astype(jnp.float32)
    inner_prod = inner_ext * input_ext
    conv_out = jnp.zeros((conv_inner.shape[0], tok_count), jnp.float32)
    for offset in range(taps_count):
        conv_out = (
            conv_out + conv_taps[offset][:, None] * inner_prod[:, offset : offset + tok_count]
        )
    outer_f = conv_outer.astype(jnp.float32)
    mixer_act = (outer_f * conv_out).astype(jnp.bfloat16)
    full_back = lax.all_gather(grad_mixed, "tp", axis=1, tiled=True)
    back_mixer = jnp.einsum("cd,td->ct", out_proj, full_back, preferred_element_type=jnp.float32)
    proj_term = jnp.dot(mixer_act, full_back, preferred_element_type=jnp.float32)
    grad_proj = lax.psum_scatter(
        proj_term.astype(jnp.bfloat16), "sp", scatter_dimension=1, tiled=True
    ).astype(jnp.float32)
    grad_outer = (back_mixer * conv_out).astype(jnp.bfloat16)
    back_conv = back_mixer * outer_f
    tail_back = from_behind(back_conv[:, :rim_width], "sp", -1)
    back_ext = jnp.concatenate([back_conv, tail_back], axis=1)
    back_prod = jnp.zeros_like(back_conv)
    for offset in range(taps_count):
        shift_by = rim_width - offset
        back_prod = (
            back_prod + conv_taps[offset][:, None] * back_ext[:, shift_by : shift_by + tok_count]
        )
    grad_inner = (back_prod * conv_input.astype(jnp.float32)).astype(jnp.bfloat16)
    grad_input = (back_prod * conv_inner.astype(jnp.float32)).astype(jnp.bfloat16)
    return (
        grad_gate_e[None],
        grad_up_e[None],
        grad_down_e[None],
        grad_mixed,
        grad_proj,
        grad_outer,
        grad_inner,
        grad_input,
    )


def solution(mesh):
    placed = (
        P("tp", "sp"),
        P("tp", "sp"),
        P("tp", "sp"),
        P(None, "tp"),
        P("tp", None),
        P("sp", "tp"),
        P("sp", None),
        P("sp", None),
        P("sp", "tp", None),
        P("sp", "tp", None),
        P("sp", "tp", None),
        P("sp", "tp"),
    )
    return jax.shard_map(
        shards,
        mesh=mesh,
        in_specs=placed,
        out_specs=(
            P("sp", "tp", None),
            P("sp", "tp", None),
            P("sp", "tp", None),
            P("sp", "tp"),
            P("tp", "sp"),
            P("tp", "sp"),
            P("tp", "sp"),
            P("tp", "sp"),
        ),
        check_vma=False,
    )
```
